32 devices in a mesh: ep: 32 (over z, y, x, core).
Axes of the slice: x: 2, y: 2, z: 4, core: 2. Of those that a mesh axis runs over, the one named last changes fastest.
Arguments:
- hidden_in: bfloat16 [512, 2048], P('ep'), may hold values from -6 to 6
- lengths: int32 [512], P('ep'), may hold values from 1 to 1024
- attn_gain: float32 [2048], replicated, may hold values from 0.1 to 1.9
- query_weight: bfloat16 [2048, 512], replicated, may hold values from -0.125 to 0.125
- key_weight: bfloat16 [2048, 128], replicated, may hold values from -0.125 to 0.125
- value_weight: bfloat16 [2048, 128], replicated, may hold values from -0.125 to 0.125
- score_bias: float32 [8], replicated, may hold values from -7.5 to -3.5
- out_weight: bfloat16 [512, 2048], replicated, may hold values from -0.25 to 0.25
- key_cache: bfloat16 [512, 1024, 128], P('ep'), may hold values from -6 to 6
- value_cache: bfloat16 [512, 1024, 128], P('ep'), may hold values from -10 to 10
- ffn_gain: float32 [2048], replicated, may hold values from 0.1 to 1.9
- routes: int32 [512, 4], P('ep'), may hold values from 0 to 31, all different within a row; in each aligned block of 16 rows (0 to 15, 16 to 31, ...) at most 2 rows name the same one
- route_weights: float32 [512, 4], P('ep'), may hold values from 0.25 to 1
- expert_gate: bfloat16 [32, 2048, 512], P('ep'), may hold values from -0.125 to 0.125
- expert_up: bfloat16 [32, 2048, 512], P('ep'), may hold values from -0.125 to 0.125
- expert_down: bfloat16 [32, 512, 2048], P('ep'), may hold values from -0.25 to 0.25
- dense_gate: bfloat16 [2048, 2048], P(None, 'ep'), may hold values from -0.125 to 0.125
- dense_up: bfloat16 [2048, 2048], P(None, 'ep'), may hold values from -0.125 to 0.125
- dense_down: bfloat16 [2048, 2048], P(None, 'ep'), may hold values from -0.125 to 0.125
- branch_gate: float32 [2048], replicated, may hold values from -0.125 to 0.125
Outputs:
- hidden_out: bfloat16 [512, 2048], P('ep')
- new_keys: bfloat16 [512, 128], P('ep')
- new_values: bfloat16 [512, 128], P('ep')
The draws below stay inside these ranges and needn't reach their ends.
Inputs may be any that keep to these rules, and one draw needn't show every extreme that they name: `routes`: in each device's 16 rows no expert is named twice.
All inputs are finite; a program needn't handle non-finite values.
Results may differ from the reference program's by a relative error of at most 0.0061.
Values may be sent and summed in bfloat16 or wider, within the bound.
A program may use at most 128 MiB of HBM per device.

```python
import math
import jax
import jax.numpy as jnp
import numpy as np
from jax import lax

D = 2048
HEADS = 8
KV_HEADS = 2
HEAD = 64
LEN = 1024
EFF = 512
TOP = 4
FDENSE = 2048
SEQ_DEV = 16
CAP = 2
BATCH = 512
EXPERTS = 32


def draw_score_bias(key, part):
    base_key = jax.random.fold_in(key, 11)
    key_slow, key_fast, key_pick = jax.random.split(base_key, 3)
    slow_bias = jax.random.uniform(key_slow, (HEADS,), jnp.float32, -7.5, -6.5)
    fast_bias = jax.random.uniform(key_fast, (HEADS,), jnp.float32, -4.5, -3.5)
    head_order = jax.random.permutation(key_pick, HEADS)
    fast_heads = head_order < HEADS // 2
    return jnp.where(fast_heads, fast_bias, slow_bias)


def draw_value_cache(key, part):
    base_key = jax.random.fold_in(key, 23)
    key_noise, key_block, key_common = jax.random.split(base_key, 3)
    row_width = KV_HEADS * HEAD
    noise_part = jax.random.normal(key_noise, (BATCH, LEN, row_width), jnp.float32)
    block_means = jax.random.normal(key_block, (BATCH, 8, row_width), jnp.float32)
    span_means = jnp.repeat(block_means, LEN // 8, axis=1)
    values_out = noise_part + span_means
    return jnp.clip(values_out, -10.0, 10.0).astype(jnp.bfloat16)


def place_ends(values, key, smallest, high):
    extent = values.shape
    place = [jax.random.randint(jax.random.fold_in(key, axis), (), 0, extent[axis]) for axis in range(len(extent))]
    values = values.at[tuple(place)].set(smallest)
    longest = extent.index(max(extent))
    place[longest] = (place[longest] + 1) % extent[longest]
    return values.at[tuple(place)].set(high)


def block_scale(stream_key, extent, cuts, smallest, largest):
    loudness = 1.0
    for position, blocks in cuts:
        steps = jax.random.uniform(jax.random.fold_in(jax.random.fold_in(stream_key, 6), position), (blocks,), jnp.float32, smallest / len(cuts), largest / len(cuts))
        loudness = loudness * jnp.repeat(jnp.exp(steps), extent[position] // blocks).reshape((-1,) + (1,) * (len(extent) - 1 - position))
    return loudness


def deal_out(key, own, number, rows, number_of, top, most, slope):
    sequence = jax.random.permutation(key, number_of)
    heavy_load, common = shares(number_of, rows * top, most, slope, True), shares(number_of, rows * top, most, slope, False)
    places = jnp.arange(number_of)

    def named(sizes, turn):
        used = int((sizes > 0).sum())
        fixed = max(1, used // 4)
        moved = fixed + (places - fixed + turn * (used - fixed)) % max(1, number_of - fixed)
        return jnp.zeros((number_of,), jnp.int32).at[sequence[jnp.where(places < fixed, places, moved)]].set(jnp.asarray(sizes, jnp.int32))

    sizes = jnp.where(number % 4 == 0, named(heavy_load, number // 4), named(common, number - number // 4 - 1))
    mixed = jax.random.permutation(jax.random.fold_in(own, 3), number_of)
    giver, receiver = mixed[0:number_of // 2 * 2:2], mixed[1:number_of // 2 * 2:2]
    slack = jnp.minimum(sizes[giver] - 1, most - sizes[receiver]) // 2
    slack = jnp.where((giver == sequence[0]) | (receiver == sequence[0]) | (sizes[receiver] == 0), 0, jnp.maximum(slack, 0))
    moved = jax.random.randint(jax.random.fold_in(own, 4), (number_of // 2,), 0, 1 << 20) % (slack + 1)
    sizes = sizes.at[giver].add(-moved).at[receiver].add(moved)
    items = jnp.searchsorted(jnp.cumsum(sizes), jnp.arange(rows * top), side="right").astype(jnp.int32)
    grid = items.reshape(top, rows).T
    grid = grid[jax.random.permutation(jax.random.fold_in(own, 1), rows)]
    turn = jax.random.randint(jax.random.fold_in(own, 2), (rows, 1), 0, top)
    return jnp.take_along_axis(grid, (jnp.arange(top)[None, :] + turn) % top, axis=1)


def shares(count, total, most, skew, full):
    weights = [(1 << 20) // math.isqrt(grade ** skew) + 1 for grade in range(1, count + 1)]
    largest = most if full else min(most, max(-(-total // count), total * weights[0] // sum(weights)))
    least = 1 if total - largest >= count - 1 else 0
    counts, rest = [largest] + [least] * (count - 1), total - largest - least * (count - 1)
    while rest > 0:
        candidates = [i for i in range(1, count) if counts[i] < largest] or [i for i in range(1, count) if counts[i] < most]
        whole, left = sum([weights[i] for i in candidates]), rest
        for i in candidates:
            extra = min(most - counts[i], max(1, left * weights[i] // whole), rest)
            counts[i] = counts[i] + extra
            rest = rest - extra
    return np.array(counts)


def normal_values(own_key, extent, spread, most, cuts=(), kind=jnp.bfloat16):
    drawn = jax.random.normal(own_key, extent, jnp.float32) * spread
    if len(cuts) > 0:
        drawn = block_scale(own_key, extent, cuts, -0.22, 0.18) * drawn
    return jnp.clip(drawn, min=-most, max=most).astype(kind)


def setup_inputs(seed: int = 0) -> dict:
    seeds = jax.random.split(jax.random.key(seed), 21)
    hidden_in = normal_values(seeds[0], (BATCH, D), 1.0, 6.0, ((0, 32),))
    lengths = place_ends(jax.random.randint(seeds[1], (BATCH,), 1, LEN + 1), jax.random.fold_in(seeds[1], 1), 1, LEN).astype(jnp.int32)
    attn_gain = jnp.clip(1.0 + 0.18 * jax.random.normal(seeds[2], (D,), jnp.float32), 0.1, 1.9)
    query_weight = normal_values(seeds[3], (D, HEADS * HEAD), D ** -0.5, 0.125)
    key_weight = normal_values(seeds[4], (D, KV_HEADS * HEAD), D ** -0.5, 0.125)
    value_weight = normal_values(seeds[5], (D, KV_HEADS * HEAD), D ** -0.5, 0.125)
    score_bias = draw_score_bias(jax.random.fold_in(seeds[20], 71), 0)
    out_weight = normal_values(seeds[7], (HEADS * HEAD, D), (HEADS * HEAD) ** -0.5, 0.25)
    key_cache = normal_values(seeds[8], (BATCH, LEN, KV_HEADS * HEAD), 1.0, 6.0, ((0, 32),))
    value_cache = draw_value_cache(jax.random.fold_in(seeds[20], 71), 0)
    ffn_gain = jnp.clip(1.0 + 0.18 * jax.random.normal(seeds[10], (D,), jnp.float32), 0.1, 1.9)
    routes_keys = jax.random.split(jax.random.fold_in(seeds[11], 1), BATCH // SEQ_DEV)
    routes_turns = jax.random.permutation(jax.random.fold_in(seeds[11], 3), BATCH // SEQ_DEV)
    routes = jax.vmap(lambda own, number: deal_out(jax.random.fold_in(seeds[11], 2), own, number, SEQ_DEV, EXPERTS, TOP, CAP, 2))(routes_keys, routes_turns).reshape((BATCH, TOP))
    route_weights = jnp.clip(0.25 + 0.75 * jax.random.uniform(seeds[12], (BATCH, TOP), jnp.float32) ** block_scale(seeds[12], (BATCH, TOP), ((0, 32),), -0.2, 0.2), 0.25, 1.0)
    expert_gate = normal_values(seeds[13], (EXPERTS, D, EFF), D ** -0.5, 0.125, ((0, 32),))
    expert_up = normal_values(seeds[14], (EXPERTS, D, EFF), D ** -0.5, 0.125, ((0, 32),))
    expert_down = normal_values(seeds[15], (EXPERTS, EFF, D), EFF ** -0.5, 0.25, ((0, 32),))
    dense_gate = normal_values(seeds[16], (D, FDENSE), D ** -0.5, 0.125, ((1, 32),))
    dense_up = normal_values(seeds[17], (D, FDENSE), D ** -0.5, 0.125, ((1, 32),))
    dense_down = normal_values(seeds[18], (D, FDENSE), FDENSE ** -0.5, 0.125, ((1, 32),))
    branch_gate = normal_values(seeds[19], (D,), D ** -0.5, 0.125, (), jnp.float32)
    return dict(hidden_in=hidden_in, lengths=lengths, attn_gain=attn_gain, query_weight=query_weight, key_weight=key_weight, value_weight=value_weight, score_bias=score_bias, out_weight=out_weight, key_cache=key_cache, value_cache=value_cache, ffn_gain=ffn_gain, routes=routes, route_weights=route_weights, expert_gate=expert_gate, expert_up=expert_up, expert_down=expert_down, dense_gate=dense_gate, dense_up=dense_up, dense_down=dense_down, branch_gate=branch_gate)


norm_eps = 1e-06

def rms_norm(values_in, gain):
    as_float = values_in.astype(jnp.float32)
    scaled = as_float * lax.rsqrt(lax.optimization_barrier(jnp.mean(as_float * as_float, axis=-1, keepdims=True)) + norm_eps)
    return (scaled * gain).astype(jnp.bfloat16)

def stick_attend(query_blk, key_blk, value_blk, seq_lens, score_bias):
    seq_count = query_blk.shape[0]
    per_group = HEADS // KV_HEADS
    query_f = query_blk.astype(jnp.float32).reshape(seq_count, KV_HEADS, per_group, HEAD)
    key_f = key_blk.astype(jnp.float32).reshape(seq_count, LEN, KV_HEADS, HEAD)
    value_f = value_blk.astype(jnp.float32).reshape(seq_count, LEN, KV_HEADS, HEAD)
    head_bias = score_bias.astype(jnp.float32).reshape(KV_HEADS, per_group)[None, :, :, None]
    scores = jnp.einsum('nkgd,nskd->nkgs', query_f, key_f) * HEAD ** (-0.5) + head_bias
    live_mask = (jnp.arange(LEN, dtype=jnp.int32)[None, :] < seq_lens[:, None])[:, None, None, :]
    log_keep = jnp.where(live_mask, jax.nn.log_sigmoid(-scores), 0.0)
    after_sum = lax.cumsum(log_keep, axis=3, reverse=True) - log_keep
    weights = jnp.where(live_mask, jnp.exp(jax.nn.log_sigmoid(scores) + after_sum), 0.0).astype(jnp.bfloat16)
    weights = lax.optimization_barrier(weights)
    mixed = jnp.einsum('nkgs,nskd->nkgd', weights.astype(jnp.float32), value_f)
    return mixed.astype(jnp.bfloat16).reshape(seq_count, HEADS * HEAD)

def reference(hidden_in, lengths, attn_gain, query_weight, key_weight, value_weight, score_bias, out_weight, key_cache, value_cache, ffn_gain, routes, route_weights, expert_gate, expert_up, expert_down, dense_gate, dense_up, dense_down, branch_gate):
    normed = rms_norm(hidden_in, attn_gain)
    queries = jnp.dot(normed, query_weight, preferred_element_type=jnp.float32).astype(jnp.bfloat16)
    new_keys = jnp.dot(normed, key_weight, preferred_element_type=jnp.float32).astype(jnp.bfloat16)
    new_values = jnp.dot(normed, value_weight, preferred_element_type=jnp.float32).astype(jnp.bfloat16)
    blocks = BATCH // SEQ_DEV

    def attend_block(pieces):
        return stick_attend(pieces[0], pieces[1], pieces[2], pieces[3], score_bias)
    attended = lax.map(attend_block, (queries.reshape(blocks, SEQ_DEV, HEADS * HEAD), key_cache.reshape(blocks, SEQ_DEV, LEN, KV_HEADS * HEAD), value_cache.reshape(blocks, SEQ_DEV, LEN, KV_HEADS * HEAD), lengths.reshape(blocks, SEQ_DEV)))
    attended = attended.reshape(BATCH, HEADS * HEAD)
    middle = hidden_in.astype(jnp.float32) + jnp.dot(attended, out_weight, preferred_element_type=jnp.float32)
    ffn_in = rms_norm(middle, ffn_gain)

    def one_token(pieces):
        token_row, expert_ids, pick_weights = pieces
        row_f = token_row.astype(jnp.float32)
        gate_pre = jnp.einsum('d,kdf->kf', row_f, expert_gate[expert_ids].astype(jnp.float32))
        up_pre = jnp.einsum('d,kdf->kf', row_f, expert_up[expert_ids].astype(jnp.float32))
        hidden_act = lax.optimization_barrier((jax.nn.silu(gate_pre) * up_pre).astype(jnp.bfloat16))
        expert_rows = jnp.einsum('kf,kfd->kd', hidden_act.astype(jnp.float32), expert_down[expert_ids].astype(jnp.float32)).astype(jnp.bfloat16)
        expert_rows = lax.optimization_barrier(expert_rows)
        return lax.optimization_barrier(jnp.sum(pick_weights[:, None] * expert_rows.astype(jnp.float32), axis=0))
    expert_sum = lax.map(one_token, (ffn_in, routes, route_weights))
    gate_pre = jnp.dot(ffn_in, dense_gate, preferred_element_type=jnp.float32)
    up_pre = jnp.dot(ffn_in, dense_up, preferred_element_type=jnp.float32)
    dense_hidden = (jax.nn.silu(gate_pre) * up_pre).astype(jnp.bfloat16)
    dense_out = jnp.dot(dense_hidden, dense_down.T, preferred_element_type=jnp.float32)
    gate_value = jax.nn.sigmoid(jnp.dot(ffn_in.astype(jnp.float32), branch_gate, precision=lax.Precision.HIGHEST))
    hidden_out = (middle + expert_sum + gate_value[:, None] * dense_out).astype(jnp.bfloat16)
    return (hidden_out, new_keys, new_values)
```

```python
import functools

import jax
import jax.numpy as jnp
from jax import lax
from jax.experimental import pallas as pl
from jax.experimental.pallas import tpu as pltpu
from jax.sharding import PartitionSpec as P

HEADS = 8
KV_HEADS = 2
HEAD = 64
TOP = 4
EXTRA = 128
SPAN = 256
GROUP = 8
MESH = pl.DeviceIdType.MESH
F32 = jnp.float32
BF16 = jnp.bfloat16

norm_eps = 1e-06


def rms_norm(as_float, gain):
    scaled = as_float * lax.rsqrt(jnp.mean(as_float * as_float, axis=-1, keepdims=True) + norm_eps)
    return (scaled * gain).astype(BF16)


def three_parts(value):
    high = value.astype(BF16)
    rest = value - high.astype(F32)
    mid = rest.astype(BF16)
    low = (rest - mid.astype(F32)).astype(BF16)
    return high, mid, low


def dot(a, b):
    return jnp.dot(a, b, preferred_element_type=F32)


def dot_t(a, b):
    return lax.dot_general(a, b, (((1,), (1,)), ((), ())), preferred_element_type=F32)


def attend_part(
    prefetch,
    lengths_hbm,
    bias_hbm,
    hidden_hbm,
    attn_gain_hbm,
    ffn_gain_hbm,
    branch_gate_hbm,
    routes_hbm,
    route_weights_hbm,
    query_w,
    key_w,
    value_w,
    out_w,
    key_c,
    value_c,
    middle_out,
    rows_out,
    keys_out,
    values_out,
    wq,
    wk,
    wv,
    wo,
    kbuf,
    vbuf,
    qs,
    zs,
    mix,
    lengths,
    bias,
    hidden,
    attn_gain,
    ffn_gain,
    branch_gate,
    routes,
    route_weights,
    small_sem,
    wsem,
    ksem,
    vsem,
):
    seqs, width = hidden.shape
    cache_len = kbuf.shape[1]
    per_group = HEADS // KV_HEADS
    kv_width = KV_HEADS * HEAD
    small = []
    for src, dst in (
        (hidden_hbm, hidden),
        (attn_gain_hbm, attn_gain),
        (lengths_hbm, lengths),
        (bias_hbm, bias),
        (ffn_gain_hbm, ffn_gain),
        (branch_gate_hbm, branch_gate),
        (routes_hbm, routes),
        (route_weights_hbm, route_weights),
    ):
        small.append(pltpu.make_async_copy(src, dst, small_sem.at[len(small)]))
        small[-1].start()
    copies = []
    for i, (src, dst) in enumerate(((query_w, wq), (key_w, wk), (value_w, wv))):
        copies.append(pltpu.make_async_copy(src, dst, wsem.at[i]))
    group = min(GROUP, seqs)
    groups = seqs // group
    kcopies, vcopies = [], []
    for b in range(seqs // 2):
        pair = pl.ds(2 * b, 2)
        kcopies.append(pltpu.make_async_copy(key_c.at[pair], kbuf.at[pair], ksem.at[b]))
        vcopies.append(pltpu.make_async_copy(value_c.at[pair], vbuf.at[pair], vsem.at[b]))
    wo_copy = pltpu.make_async_copy(out_w, wo, wsem.at[3])

    def fetch(g):
        for copy in kcopies[g * group // 2 : (g + 1) * group // 2]:
            copy.start()
        for copy in vcopies[g * group // 2 : (g + 1) * group // 2]:
            copy.start()

    copies[0].start()
    fetch(0)
    small[0].wait()
    small[1].wait()
    hidden_f = hidden[...].astype(F32)
    normed = rms_norm(hidden_f, attn_gain[...])
    copies[0].wait()
    for g in range(1, groups):
        fetch(g)
    wo_copy.start()
    copies[1].start()
    copies[2].start()
    queries = dot(normed, wq[...]).astype(BF16).astype(F32) * HEAD ** (-0.5)
    lane = lax.broadcasted_iota(jnp.int32, (seqs, kv_width), 1)
    for h in range(HEADS):
        tile = queries[:, (h // 2) * kv_width : (h // 2 + 1) * kv_width]
        if h % 2 != h // per_group:
            tile = pltpu.roll(tile, HEAD, 1)
        qs[:, h, :] = jnp.where(lane // HEAD == h // per_group, tile, 0.0)
    small[2].wait()
    small[3].wait()

    pos_r = lax.broadcasted_iota(jnp.int32, (SPAN, SPAN), 0)
    pos_c = lax.broadcasted_iota(jnp.int32, (SPAN, SPAN), 1)
    tri = (pos_r >= pos_c).astype(F32).astype(BF16)
    position = lax.broadcasted_iota(jnp.int32, (HEADS, cache_len), 1)
    head_row = lax.broadcasted_iota(jnp.int32, (HEADS, cache_len), 0)
    head_bias = jnp.zeros((HEADS, cache_len), F32)
    for h in range(HEADS):
        head_bias = jnp.where(head_row == h, bias[h], head_bias)
    spans = cache_len // SPAN
    blank = jnp.zeros((HEADS, kv_width), F32)
    for g in range(groups):
        members = range(g * group, (g + 1) * group)
        for b in members[::2]:
            kcopies[b // 2].wait()
        keeps = []
        for b in members[::2]:
            both = jnp.concatenate(
                [jnp.concatenate([qs[b], blank], axis=1), jnp.concatenate([blank, qs[b + 1]], axis=1)], axis=0
            ).astype(BF16)
            scores = dot_t(both, jnp.concatenate([kbuf[b], kbuf[b + 1]], axis=1))
            for i in range(2):
                z = scores[i * HEADS : (i + 1) * HEADS] + head_bias
                zs[b + i] = z
                soft = jnp.maximum(z, 0.0) + jnp.log(1.0 + jnp.exp(-jnp.abs(z)))
                keeps.append(jnp.where(position < lengths[b + i], soft, 0.0))
        parts = jnp.concatenate(three_parts(jnp.concatenate(keeps, axis=0)), axis=0)
        rows = group * HEADS
        carry = jnp.zeros((rows, 1), F32)
        suffix = [None] * spans
        for s in reversed(range(spans)):
            sums = dot(parts[:, s * SPAN : (s + 1) * SPAN], tri)
            inside = sums[:rows] + sums[rows : 2 * rows] + sums[2 * rows :]
            suffix[s] = inside + carry
            carry = carry + inside[:, :1]
        suffix = jnp.concatenate(suffix, axis=1)
        ws = []
        for i, b in enumerate(members):
            log_w = zs[b] - suffix[i * HEADS : (i + 1) * HEADS]
            ws.append(jnp.where(position < lengths[b], jnp.exp(log_w), 0.0))
        for b in members[::2]:
            vcopies[b // 2].wait()
        for i, b in enumerate(members[::2]):
            both = jnp.concatenate(ws[2 * i : 2 * i + 2], axis=0).astype(BF16)
            mixed = dot(both, jnp.concatenate([vbuf[b], vbuf[b + 1]], axis=1))
            mix[b] = mixed[:HEADS, :kv_width]
            mix[b + 1] = mixed[HEADS:, kv_width:]
        if g == 0:
            prefetch()
    copies[1].wait()
    keys_out[...] = dot(normed, wk[...]).astype(BF16)
    copies[2].wait()
    values_out[...] = dot(normed, wv[...]).astype(BF16)
    tiles = []
    for t in range(HEADS // 2):
        pieces = []
        for h in (2 * t, 2 * t + 1):
            tile = mix[:, h, :]
            if h % 2 != h // per_group:
                tile = pltpu.roll(tile, HEAD, 1)
            pieces.append(tile)
        tiles.append(jnp.where(lane < HEAD, pieces[0], pieces[1]))
    attended = jnp.concatenate(tiles, axis=1).astype(BF16)
    wo_copy.wait()
    middle = hidden_f + dot(attended, wo[...])
    middle_out[...] = middle
    for copy in small[4:]:
        copy.wait()
    ffn_in = rms_norm(middle, ffn_gain[...])
    rows_out[:, :width] = ffn_in
    gate = jax.nn.sigmoid(jnp.sum(ffn_in.astype(F32) * branch_gate[...], axis=1, keepdims=True))
    by_row = [routes[...].astype(F32)] + [part.astype(F32) for part in three_parts(route_weights[...])]
    by_row.append(jnp.zeros((EXTRA - 4 * TOP, seqs), F32))
    by_row = jnp.concatenate(by_row, axis=0)
    extra = jnp.concatenate([by_row, jnp.zeros((EXTRA, EXTRA - seqs), F32)], axis=1).T[:seqs]
    extra_lane = lax.broadcasted_iota(jnp.int32, (seqs, EXTRA), 1)
    for i, part in enumerate(three_parts(gate)):
        extra = jnp.where(extra_lane == 4 * TOP + i, part.astype(F32), extra)
    rows_out[:, width:] = extra.astype(BF16)


def flip(v, j):
    if j == 0:
        return v
    if j == 1:
        return v + 1 - 2 * (v % 2)
    if j == 2:
        return (v + 2) % 4
    return 3 - v


def layer_kernel(dims, cap, *refs):
    attend_in, ffn_in, whole, refs = refs[:14], refs[14:20], refs[20], refs[21:]
    width = ffn_in[3].shape[1]
    kv_width = KV_HEADS * HEAD
    outs = [
        whole.at[:, pl.ds(0, width)],
        whole.at[:, pl.ds(width, kv_width)],
        whole.at[:, pl.ds(width + kv_width, kv_width)],
    ]
    attend_scratch, ffn_scratch = refs[:21], refs[21:]

    def attend(prefetch, middle, rows):
        attend_part(prefetch, *attend_in, middle, rows, *outs[1:], *attend_scratch)

    ffn_part(dims, cap, attend, *ffn_in, outs[0], *ffn_scratch)


def ffn_part(
    dims,
    cap,
    attend,
    eg_hbm,
    eu_hbm,
    ed_hbm,
    dg_hbm,
    du_hbm,
    dd_hbm,
    out,
    middle,
    rows,
    eg,
    eu,
    ed,
    dg,
    du,
    dd,
    buf,
    part,
    rcore,
    summed,
    rx,
    ry,
    qa,
    qb,
    rya,
    rxb,
    tsum,
    rz,
    wsem,
    s_sem,
    r_sem,
):
    C, Z, Y, X = dims
    seqs, width = middle.shape
    half = width // 2
    me = lax.axis_index("ep")
    c = me % C
    x = (me // C) % X
    y = (me // (C * X)) % Y
    z = me // (C * X * Y)

    def dev(zz, yy, xx, cc):
        return (((zz * Y + yy) * X + xx) * C + cc,)

    z_mates = [dev(flip(z, j), y, x, c) for j in range(1, Z)]
    y_mates = [dev(z, flip(y, o), x, c) for o in range(1, Y)]
    x_mates = [dev(z, y, flip(x, o), c) for o in range(1, X)]
    peer = dev(z, y, x, 1 - c)
    barrier = pltpu.get_barrier_semaphore()
    mates = z_mates + y_mates + x_mates + [peer]
    for mate in mates:
        pl.semaphore_signal(barrier, inc=1, device_id=mate, device_id_type=MESH)
    weight_copies = []

    def prefetch():
        for i, (src, dst) in enumerate(
            ((dg_hbm, dg), (du_hbm, du), (eg_hbm, eg), (eu_hbm, eu), (ed_hbm, ed), (dd_hbm, dd))
        ):
            weight_copies.append(pltpu.make_async_copy(src, dst, wsem.at[i]))
            weight_copies[-1].start()

    attend(prefetch, middle, rows)
    pl.semaphore_wait(barrier, len(mates))

    sent = []
    count = [0]

    def send(src, dst, where):
        k = count[0]
        count[0] += 1
        copy = pltpu.make_async_remote_copy(
            src_ref=src,
            dst_ref=dst,
            send_sem=s_sem.at[k],
            recv_sem=r_sem.at[k],
            device_id=where,
            device_id_type=MESH,
        )
        copy.start()
        sent.append(copy)
        return copy

    A = pl.ds(0, half)
    B = pl.ds(half, width + EXTRA - half)
    B_out = pl.ds(half, width - half)
    z_copies = {}
    for j in range(1, Z):
        z_copies[j] = send(rows, buf.at[c, z, y, x], z_mates[j - 1])
    buf[c, z, y, x] = rows[...]

    blocks = C * Y * X
    group_rows = blocks * seqs
    state = [dict() for _ in range(Z)]

    def spread_first(j):
        zj = flip(z, j)
        if j:
            z_copies[j].wait_recv()
        src = buf.at[c, zj, y, x] if j else rows
        state[j]["y"] = [send(src.at[:, A], buf.at[c, zj, y, x, :, A], mate) for mate in y_mates]
        state[j]["x"] = [send(src.at[:, B], buf.at[c, zj, y, x, :, B], mate) for mate in x_mates]

    def spread_second(j):
        zj = flip(z, j)
        for copy in state[j]["y"]:
            copy.wait_recv()
        spot = buf.at[c, zj, :, x, :, A]
        xs = [send(spot, spot, mate) for mate in x_mates]
        for copy in state[j]["x"]:
            copy.wait_recv()
        spot = buf.at[c, zj, y, :, :, B]
        state[j]["second"] = xs + [send(spot, spot, mate) for mate in y_mates]

    def spread_core(j):
        zj = flip(z, j)
        for copy in state[j]["second"]:
            copy.wait_recv()
        spot = buf.at[c, zj]
        state[j]["core"] = send(spot, spot, peer)

    row_i = lax.broadcasted_iota(jnp.int32, (group_rows, group_rows), 0)
    col_i = lax.broadcasted_iota(jnp.int32, (group_rows, group_rows), 1)
    earlier = ((row_i // seqs == col_i // seqs) & (row_i < col_i)).astype(F32).astype(BF16)
    slots = blocks * cap
    slot_i = lax.broadcasted_iota(jnp.int32, (slots, group_rows), 0)
    slot_block = lax.broadcasted_iota(jnp.int32, (slots, group_rows), 1) // seqs

    def compute(j):
        zj = flip(z, j)
        state[j]["core"].wait_recv()
        got = buf[:, zj].reshape(group_rows, width + EXTRA)
        tokens = got[:, :width]
        extra = got[:, width:].astype(F32)
        gate = extra[:, 4 * TOP : 4 * TOP + 1] + extra[:, 4 * TOP + 1 : 4 * TOP + 2] + extra[:, 4 * TOP + 2 : 4 * TOP + 3]
        flat = extra.T
        if j == 0:
            weight_copies[0].wait()
            weight_copies[1].wait()
        dense_gate = dot_t(tokens, dg[...])
        dense_up = dot_t(tokens, du[...])
        dense = (dense_gate / (1.0 + jnp.exp(-dense_gate)) * dense_up * gate).astype(BF16)
        hit = (flat[0:TOP] == me.astype(F32)).astype(F32)
        weight = flat[TOP : 2 * TOP] + flat[2 * TOP : 3 * TOP] + flat[3 * TOP : 4 * TOP]
        named = jnp.sum(hit, axis=0, keepdims=True)
        row_weight = jnp.sum(hit * weight, axis=0, keepdims=True)
        ranks = dot(jnp.broadcast_to(named, (16, group_rows)).astype(BF16), earlier)[0:1]
        slot = slot_block * cap + ranks.astype(jnp.int32)
        pick = jnp.where((slot == slot_i) & (named > 0.0), 1.0, 0.0)
        slot_weight = jnp.sum(pick * row_weight, axis=1, keepdims=True)
        pick = pick.astype(BF16)
        picked = dot(pick, tokens).astype(BF16)
        if j == 0:
            weight_copies[2].wait()
            weight_copies[3].wait()
        gate_pre = dot(picked, eg[0])
        up_pre = dot(picked, eu[0])
        act = (gate_pre / (1.0 + jnp.exp(-gate_pre)) * up_pre).astype(BF16)
        if j == 0:
            weight_copies[4].wait()
            weight_copies[5].wait()
        expert = dot(act, ed[0]).astype(BF16).astype(F32)
        expert = (expert * slot_weight).astype(BF16)
        total = dot(dense, dd[...]) + lax.dot_general(
            pick, expert, (((0,), (0,)), ((), ())), preferred_element_type=F32
        )
        part[:, j] = total.astype(BF16).reshape(C, Y, X, seqs, width)
        state[j]["rc"] = send(part.at[1 - c, j], rcore.at[j], peer)

    def reduce_core(j):
        state[j]["rc"].wait_recv()
        summed[j] = (part[c, j].astype(F32) + rcore[j].astype(F32)).astype(BF16)
        state[j]["rx"] = [
            send(summed.at[j, :, flip(x, o), :, A], rx.at[j, o - 1], x_mates[o - 1]) for o in range(1, X)
        ]
        state[j]["ry"] = [
            send(summed.at[j, flip(y, o), :, :, B_out], ry.at[j, o - 1], y_mates[o - 1]) for o in range(1, Y)
        ]

    def reduce_first(j):
        total = summed[j, :, x, :, :half].astype(F32)
        for o, copy in enumerate(state[j]["rx"]):
            copy.wait_recv()
            total = total + rx[j, o].astype(F32)
        qa[j] = total.astype(BF16)
        state[j]["rya"] = [send(qa.at[j, flip(y, o)], rya.at[j, o - 1], y_mates[o - 1]) for o in range(1, Y)]
        total = summed[j, y, :, :, half:].astype(F32)
        for o, copy in enumerate(state[j]["ry"]):
            copy.wait_recv()
            total = total + ry[j, o].astype(F32)
        qb[j] = total.astype(BF16)
        state[j]["rxb"] = [send(qb.at[j, flip(x, o)], rxb.at[j, o - 1], x_mates[o - 1]) for o in range(1, X)]

    def reduce_second(j):
        total_a = qa[j, y].astype(F32)
        for o, copy in enumerate(state[j]["rya"]):
            copy.wait_recv()
            total_a = total_a + rya[j, o].astype(F32)
        total_b = qb[j, x].astype(F32)
        for o, copy in enumerate(state[j]["rxb"]):
            copy.wait_recv()
            total_b = total_b + rxb[j, o].astype(F32)
        if j:
            tsum[j, :, :half] = total_a.astype(BF16)
            tsum[j, :, half:] = total_b.astype(BF16)
            state[j]["z"] = send(tsum.at[j], rz.at[j], z_mates[j - 1])
        else:
            state[j]["own"] = (total_a, total_b)

    stages = (spread_first, spread_second, spread_core, compute, reduce_core, reduce_first, reduce_second)
    order = list(range(Z))
    for t in range(len(stages) + Z - 1):
        for s, stage in enumerate(stages):
            if 0 <= t - s < Z:
                stage(order[t - s])
    total_a, total_b = state[0]["own"]
    total_a = total_a + middle[:, :half]
    total_b = total_b + middle[:, half:]
    for j in range(1, Z):
        state[j]["z"].wait_recv()
        total_a = total_a + rz[j, :, :half].astype(F32)
        total_b = total_b + rz[j, :, half:].astype(F32)
    out[:, :half] = total_a.astype(BF16)
    out[:, half:] = total_b.astype(BF16)
    for copy in sent:
        copy.wait_send()


def split_kernel(whole, *refs):
    outs, sem = refs[:-1], refs[-1]
    copies, start = [], 0
    for i, out in enumerate(outs):
        size = out.shape[1]
        copies.append(pltpu.make_async_copy(whole.at[:, pl.ds(start, size)], out, sem.at[i]))
        copies[-1].start()
        start += size
    for copy in copies:
        copy.wait()


def grid_of(devices):
    cores = 2
    rest = devices // cores
    z = min(rest, 4)
    rest //= z
    x = 1
    while x * x < rest:
        x *= 2
    return cores, z, rest // x, x


def per_device(
    hidden_in,
    lengths,
    attn_gain,
    query_weight,
    key_weight,
    value_weight,
    score_bias,
    out_weight,
    key_cache,
    value_cache,
    ffn_gain,
    routes,
    route_weights,
    expert_gate,
    expert_up,
    expert_down,
    dense_gate,
    dense_up,
    dense_down,
    branch_gate,
    *,
    devices,
):
    seqs, width = hidden_in.shape
    cache_len, kv_width = key_cache.shape[1:]
    vmem = pl.BlockSpec(memory_space=pltpu.VMEM)
    hbm = pl.BlockSpec(memory_space=pltpu.HBM)
    sds = jax.ShapeDtypeStruct
    dma = pltpu.SemaphoreType.DMA
    attend_scratch = [
        pltpu.VMEM(query_weight.shape, BF16),
        pltpu.VMEM(key_weight.shape, BF16),
        pltpu.VMEM(value_weight.shape, BF16),
        pltpu.VMEM(out_weight.shape, BF16),
        pltpu.VMEM(key_cache.shape, BF16),
        pltpu.VMEM(value_cache.shape, BF16),
        pltpu.VMEM((seqs, HEADS, kv_width), F32),
        pltpu.VMEM((seqs, HEADS, cache_len), F32),
        pltpu.VMEM((seqs, HEADS, kv_width), F32),
        pltpu.SMEM((seqs,), jnp.int32),
        pltpu.SMEM((HEADS,), F32),
        pltpu.VMEM((seqs, width), BF16),
        pltpu.VMEM((1, width), F32),
        pltpu.VMEM((1, width), F32),
        pltpu.VMEM((1, width), F32),
        pltpu.VMEM((TOP, seqs), jnp.int32),
        pltpu.VMEM((TOP, seqs), F32),
        dma((8,)),
        dma((4,)),
        dma((seqs,)),
        dma((seqs,)),
    ]
    dense_gate, dense_up, dense_down = dense_gate.T, dense_up.T, dense_down.T
    dims = grid_of(devices)
    C, Z, Y, X = dims
    half = width // 2
    cap = max(1, seqs * TOP // (expert_gate.shape[0] * devices))
    copies = (Z - 1) * 2 + Z * (4 * (X - 1) + 4 * (Y - 1) + 2)
    scratch = [
        expert_gate.shape,
        expert_up.shape,
        expert_down.shape,
        dense_gate.shape,
        dense_up.shape,
        dense_down.shape,
        (C, Z, Y, X, seqs, width + EXTRA),
        (C, Z, Y, X, seqs, width),
        (Z, Y, X, seqs, width),
        (Z, Y, X, seqs, width),
        (Z, max(X - 1, 1), Y, seqs, half),
        (Z, max(Y - 1, 1), X, seqs, width - half),
        (Z, Y, seqs, half),
        (Z, X, seqs, width - half),
        (Z, max(Y - 1, 1), seqs, half),
        (Z, max(X - 1, 1), seqs, width - half),
        (Z, seqs, width),
        (Z, seqs, width),
    ]
    whole = pl.pallas_call(
        functools.partial(layer_kernel, dims, cap),
        out_shape=pltpu.VMEM((seqs, width + 2 * kv_width), BF16),
        in_specs=[hbm] * 20,
        out_specs=vmem,
        scratch_shapes=attend_scratch
        + [pltpu.VMEM((seqs, width), F32), pltpu.VMEM((seqs, width + EXTRA), BF16)]
        + [pltpu.VMEM(shape, BF16) for shape in scratch]
        + [dma((6,)), dma((copies,)), dma((copies,))],
        compiler_params=pltpu.CompilerParams(
            collective_id=0,
            has_side_effects=True,
            vmem_limit_bytes=62914560,
        ),
        name="layer",
    )(
        lengths,
        score_bias,
        hidden_in,
        attn_gain.reshape(1, width),
        ffn_gain.reshape(1, width),
        branch_gate.reshape(1, width),
        routes.T,
        route_weights.T,
        query_weight,
        key_weight,
        value_weight,
        out_weight,
        key_cache,
        value_cache,
        expert_gate,
        expert_up,
        expert_down,
        dense_gate,
        dense_up,
        dense_down,
    )
    return tuple(
        pl.pallas_call(
            split_kernel,
            out_shape=[sds((seqs, size), BF16) for size in (width, kv_width, kv_width)],
            in_specs=[vmem],
            out_specs=[hbm] * 3,
            scratch_shapes=[dma((3,))],
            name="split",
        )(pltpu.with_memory_space_constraint(whole, pltpu.VMEM))
    )


def solution(mesh):
    return jax.shard_map(
        functools.partial(per_device, devices=mesh.shape["ep"]),
        mesh=mesh,
        in_specs=(
            P("ep", None),
            P("ep"),
            P(),
            P(),
            P(),
            P(),
            P(),
            P(),
            P("ep", None, None),
            P("ep", None, None),
            P(),
            P("ep", None),
            P("ep", None),
            P("ep", None, None),
            P("ep", None, None),
            P("ep", None, None),
            P(None, "ep"),
            P(None, "ep"),
            P(None, "ep"),
            P(),
        ),
        out_specs=(P("ep", None), P("ep", None), P("ep", None)),
        check_vma=False,
    )
```
